32 devices in a mesh: sp: 2 (over x), tp: 16 (over z, y, core).
Axes of the slice: x: 2, y: 2, z: 4, core: 2. Of those that a mesh axis runs over, the one named last changes fastest.
Arguments:
- query_first: bfloat16 [1024, 1536], P('sp', 'tp'), may hold values from -10 to 10
- query_second: bfloat16 [1024, 2560], P('sp', 'tp'), may hold values from -10 to 10
- latent: bfloat16 [1024, 512], P('sp'), may hold values from -400 to 400
- key_rotary: bfloat16 [1024, 32], P('sp'), may hold values from -90 to 90
- latent_gain: float32 [512], replicated, may hold values from 0.1 to 1.9
- key_up_first: bfloat16 [512, 1024], P(None, 'tp'), may hold values from -0.25 to 0.25
- value_up_first: bfloat16 [512, 1024], P(None, 'tp'), may hold values from -0.25 to 0.25
- key_up_second: bfloat16 [512, 2048], P(None, 'tp'), may hold values from -0.25 to 0.25
- value_up_second: bfloat16 [512, 2048], P(None, 'tp'), may hold values from -0.25 to 0.25
- out_first: bfloat16 [1024, 2048], P('tp'), may hold values from -0.109375 to 0.109375
- out_second: bfloat16 [2048, 2048], P('tp'), may hold values from -0.109375 to 0.109375
- residual: bfloat16 [1024, 2048], P('sp'), may hold values from -16 to 16
- expert_gain: float32 [2048], replicated, may hold values from 0.1 to 1.9
- route_experts: int32 [1024, 2], P('sp'), may hold values from 0 to 31, all different within a row; in each aligned block of 32 rows (0 to 31, 32 to 63, ...) at most 3 rows name the same one
- route_scores: float32 [1024, 2], P('sp'), may hold values from -6 to 306
- gate_weight: bfloat16 [32, 2048, 4096], P('sp', None, 'tp'), may hold values from -0.375 to 0.375
- up_weight: bfloat16 [32, 2048, 4096], P('sp', None, 'tp'), may hold values from -0.375 to 0.375
- down_weight: bfloat16 [32, 4096, 2048], P('sp', 'tp'), may hold values from -0.013671875 to 0.013671875
Outputs:
- mixed: bfloat16 [1024, 2048], P(('sp', 'tp'))
The draws below stay inside these ranges and needn't reach their ends.
Inputs may be any that keep to these rules, and one draw needn't show every extreme that they name: `route_experts`: each row names 2 different experts. In every aligned block of 32 rows no expert is named more than 3 times, and in some blocks one is named exactly 3 times.
All inputs are finite; a program needn't handle non-finite values.
Results may differ from the reference program's by a relative error of at most 0.02.
The reference program's roundings to bfloat16 on the way count: a program that leaves them out, or rounds other values in their place, can miss the bound.
Values may be sent and summed in bfloat16 or wider, within the bound.
A program may use at most 128 MiB of HBM per device.

```python
import math
import jax
import jax.numpy as jnp
import numpy as np
from jax import lax

D = 2048
HA = 16
HB = 16
NA = 64
VA = 64
NB = 128
VB = 128
ROPE = 32
RANK = 512
FF = 4096
EXPERTS = 32
TOPK = 2
CAP = 3
TOK_SP = 512
TOKENS = 1024
N_SP = 2
N_TP = 16


def scaled_field(key, rows, columns, lower, upper):
    base_key, row_key, column_key = jax.random.split(key, 3)
    base = jnp.clip(jax.random.normal(base_key, (rows, columns), jnp.float32), -4.0, 4.0)
    row_scale = jnp.exp(jax.random.uniform(row_key, (rows, 1), jnp.float32, math.log(lower), math.log(upper)))
    column_scale = jnp.exp(jax.random.uniform(column_key, (1, columns), jnp.float32, math.log(lower), math.log(upper)))
    return base * row_scale * column_scale


def draw_latent(key, part):
    return scaled_field(jax.random.fold_in(key, 11), TOKENS, RANK, 1.0, 10.0).astype(jnp.bfloat16)


def draw_residual(key, part):
    return scaled_field(jax.random.fold_in(key, 12), TOKENS, D, 0.2, 2.0).astype(jnp.bfloat16)


def draw_key_rotary(key, part):
    base_key = jax.random.fold_in(jax.random.fold_in(key, 13), 0)
    base = jnp.clip(jax.random.normal(base_key, (TOKENS, ROPE), jnp.float32), -4.0, 4.0)
    return base.astype(jnp.bfloat16)


def draw_route_scores(key, part):
    base_key = jax.random.fold_in(jax.random.fold_in(key, 14), 0)
    base = jnp.clip(1.5 * jax.random.normal(base_key, (TOKENS, TOPK), jnp.float32), -6.0, 6.0)
    return base.astype(jnp.float32)


def levels(rng, dims, pieces, least, largest):
    def one(dim, shards_of):
        draws = jax.random.uniform(jax.random.fold_in(jax.random.fold_in(rng, 6), dim), (shards_of,), jnp.float32, least / len(pieces), largest / len(pieces))
        return jnp.repeat(jnp.exp(draws), dims[dim] // shards_of).reshape((-1,) + (1,) * (len(dims) - dim - 1))

    factor_of = one(*pieces[0])
    for cut in pieces[1:]:
        factor_of = factor_of * one(*cut)
    return factor_of


def routed_block(stream_key, own, number, rows, number_of, top, bound, lean):
    sequence = jax.random.permutation(stream_key, number_of)
    crowded, ordinary = portions_of(number_of, rows * top, bound, lean, True), portions_of(number_of, rows * top, bound, lean, False)
    places = jnp.arange(number_of)

    def named(lengths, rotation):
        used = int((lengths > 0).sum())
        fixed = max(1, used // 4)
        shifted = fixed + (places - fixed + rotation * (used - fixed)) % max(1, number_of - fixed)
        return jnp.zeros((number_of,), jnp.int32).at[sequence[jnp.where(places < fixed, places, shifted)]].set(jnp.asarray(lengths, jnp.int32))

    lengths = jnp.where(number % 4 == 0, named(crowded, number // 4), named(ordinary, number - number // 4 - 1))
    mixed = jax.random.permutation(jax.random.fold_in(own, 3), number_of)
    source_of, sink = mixed[0:number_of // 2 * 2:2], mixed[1:number_of // 2 * 2:2]
    margin = jnp.minimum(lengths[source_of] - 1, bound - lengths[sink]) // 2
    margin = jnp.where((source_of == sequence[0]) | (sink == sequence[0]) | (lengths[sink] == 0), 0, jnp.maximum(margin, 0))
    shifted = jax.random.randint(jax.random.fold_in(own, 4), (number_of // 2,), 0, 1 << 20) % (margin + 1)
    lengths = lengths.at[source_of].add(-shifted).at[sink].add(shifted)
    labels = jnp.searchsorted(jnp.cumsum(lengths), jnp.arange(rows * top), side="right").astype(jnp.int32)
    grid = labels.reshape(top, rows).T
    grid = grid[jax.random.permutation(jax.random.fold_in(own, 1), rows)]
    rotation = jax.random.randint(jax.random.fold_in(own, 2), (rows, 1), 0, top)
    return jnp.take_along_axis(grid, (jnp.arange(top)[None, :] + rotation) % top, axis=1)


def portions_of(amount, total, reach, skew, full):
    loads = [(1 << 20) // math.isqrt(grade ** skew) + 1 for grade in range(1, amount + 1)]
    largest = reach if full else min(reach, max(-(-total // amount), total * loads[0] // sum(loads)))
    least = 1 if total - largest >= amount - 1 else 0
    counts, surplus = [largest] + [least] * (amount - 1), total - largest - least * (amount - 1)
    while surplus > 0:
        free = [i for i in range(1, amount) if counts[i] < largest] or [i for i in range(1, amount) if counts[i] < reach]
        mass, budget = sum([loads[i] for i in free]), surplus
        for i in free:
            addition = min(reach - counts[i], max(1, budget * loads[i] // mass), surplus)
            counts[i] = counts[i] + addition
            surplus = surplus - addition
    return np.array(counts)


def scatter_about(key, dims, scale, limit, cuts=(), kind=jnp.bfloat16):
    array = scale * jax.random.normal(key, dims, jnp.float32)
    if cuts:
        array = array * levels(key, dims, cuts, -0.22, 0.18)
    return jnp.clip(array, -limit, limit).astype(kind)


def setup_inputs(seed: int = 0) -> dict:
    key_of = jax.random.split(jax.random.key(seed), 19)
    query_first = scatter_about(key_of[0], (TOKENS, HA * (NA + ROPE)), 2.5, 10.0, ((0, 2), (1, 16)))
    query_second = scatter_about(key_of[1], (TOKENS, HB * (NB + ROPE)), 2.5, 10.0, ((0, 2), (1, 16)))
    latent = draw_latent(jax.random.fold_in(key_of[18], 71), 0)
    key_rotary = draw_key_rotary(jax.random.fold_in(key_of[18], 71), 0)
    latent_gain = jnp.clip(1.0 + 0.18 * jax.random.normal(key_of[4], (RANK,), jnp.float32), 0.1, 1.9)
    key_up_first = scatter_about(key_of[5], (RANK, HA * NA), RANK ** -0.5, 0.25, ((1, 16),))
    value_up_first = scatter_about(key_of[6], (RANK, HA * VA), RANK ** -0.5, 0.25, ((1, 16),))
    key_up_second = scatter_about(key_of[7], (RANK, HB * NB), RANK ** -0.5, 0.25, ((1, 16),))
    value_up_second = scatter_about(key_of[8], (RANK, HB * VB), RANK ** -0.5, 0.25, ((1, 16),))
    out_first = scatter_about(key_of[9], (HA * VA, D), (HA * VA + HB * VB) ** -0.5, 0.109375, ((0, 16),))
    out_second = scatter_about(key_of[10], (HB * VB, D), (HA * VA + HB * VB) ** -0.5, 0.109375, ((0, 16),))
    residual = draw_residual(jax.random.fold_in(key_of[18], 71), 0)
    expert_gain = jnp.clip(1.0 + 0.18 * jax.random.normal(key_of[12], (D,), jnp.float32), 0.1, 1.9)
    route_experts_keys = jax.random.split(jax.random.fold_in(key_of[13], 1), TOKENS // (TOK_SP // N_TP))
    route_experts_turns = jax.random.permutation(jax.random.fold_in(key_of[13], 3), TOKENS // (TOK_SP // N_TP))
    route_experts = jax.vmap(lambda own, number: routed_block(jax.random.fold_in(key_of[13], 2), own, number, TOK_SP // N_TP, EXPERTS, TOPK, CAP, 2))(route_experts_keys, route_experts_turns).reshape((TOKENS, TOPK))
    route_scores = draw_route_scores(jax.random.fold_in(key_of[18], 71), 0)
    gate_weight = scatter_about(key_of[15], (EXPERTS, D, FF), (D // 9) ** -0.5, 0.375, ((0, 2), (2, 16)))
    up_weight = scatter_about(key_of[16], (EXPERTS, D, FF), (D // 9) ** -0.5, 0.375, ((0, 2), (2, 16)))
    down_weight = scatter_about(key_of[17], (EXPERTS, FF, D), (FF * 44) ** -0.5, 0.013671875, ((0, 2), (1, 16)))
    return {"query_first": query_first, "query_second": query_second, "latent": latent, "key_rotary": key_rotary, "latent_gain": latent_gain, "key_up_first": key_up_first, "value_up_first": value_up_first, "key_up_second": key_up_second, "value_up_second": value_up_second, "out_first": out_first, "out_second": out_second, "residual": residual, "expert_gain": expert_gain, "route_experts": route_experts, "route_scores": route_scores, "gate_weight": gate_weight, "up_weight": up_weight, "down_weight": down_weight}


norm_epsilon = 1e-06
rotary_base = 10000.0
clamp_limit = 7.0
sigmoid_slope = 1.702
masked_score = -1e+30

def rotate(values, positions):
    half = values.shape[-1] // 2
    inverse = rotary_base ** (-jnp.arange(half, dtype=jnp.float32) / half)
    angles = positions.astype(jnp.float32)[:, None, None] * inverse[None, None, :]
    cosine = jnp.cos(angles)
    sine = jnp.sin(angles)
    first = values[..., :half]
    second = values[..., half:]
    return jnp.concatenate([first * cosine - second * sine, second * cosine + first * sine], axis=-1)

def rms_scaled(values, gain):
    wide = values.astype(jnp.float32)
    return wide * lax.rsqrt(lax.optimization_barrier(jnp.mean(wide * wide, axis=-1, keepdims=True)) + norm_epsilon) * gain

def turned_queries(query, nope, positions):
    shaped = query.reshape(query.shape[0], query.shape[1] // (nope + ROPE), nope + ROPE)
    turned = rotate(shaped[..., nope:].astype(jnp.float32), positions).astype(jnp.bfloat16)
    return jnp.concatenate([shaped[..., :nope], turned], axis=-1)

def clamped_unit(gate, upward):
    limited = jnp.minimum(gate, clamp_limit)
    bounded = jnp.clip(upward, -clamp_limit, clamp_limit)
    return (bounded + 1.0) * limited * jax.nn.sigmoid(sigmoid_slope * limited)

def attend_group(queries, key_nope, key_turned, values, scale):
    total = queries.shape[0]
    step_rows = math.gcd(total, 512)
    heads = queries.shape[1]
    nope = key_nope.shape[1] // heads
    keys = key_nope.reshape(total, heads, nope).astype(jnp.float32)
    value_rows = values.reshape(total, heads, values.shape[1] // heads).astype(jnp.float32)
    turned = key_turned.astype(jnp.float32)
    key_places = jnp.arange(total, dtype=jnp.int32)

    def one_block(index):
        rows = lax.dynamic_slice_in_dim(queries, index * step_rows, step_rows, 0).astype(jnp.float32)
        score = jnp.einsum('qhd,khd->qhk', rows[..., :nope], keys)
        score = (score + jnp.einsum('qhr,kr->qhk', rows[..., nope:], turned)) * scale
        places = index * step_rows + jnp.arange(step_rows, dtype=jnp.int32)
        allowed = (places[:, None] >= key_places[None, :])[:, None, :]
        score = jnp.where(allowed, score, masked_score)
        highest = lax.optimization_barrier(jnp.max(score, axis=-1, keepdims=True))
        weights = jnp.where(allowed, jnp.exp(score - highest), 0.0)
        denominator = lax.optimization_barrier(jnp.sum(weights, axis=-1))
        rounded = lax.optimization_barrier(weights.astype(jnp.bfloat16)).astype(jnp.float32)
        numerator = jnp.einsum('qhk,khd->qhd', rounded, value_rows)
        return (numerator / denominator[..., None]).astype(jnp.bfloat16)
    blocks = lax.map(one_block, jnp.arange(total // step_rows, dtype=jnp.int32))
    return blocks.reshape(total, -1)

def reference(query_first, query_second, latent, key_rotary, latent_gain, key_up_first, value_up_first, key_up_second, value_up_second, out_first, out_second, residual, expert_gain, route_experts, route_scores, gate_weight, up_weight, down_weight):
    total = latent.shape[0]
    places = jnp.arange(total, dtype=jnp.int32)
    queries_first = turned_queries(query_first, NA, places)
    queries_second = turned_queries(query_second, NB, places)
    key_turned = rotate(key_rotary.astype(jnp.float32)[:, None, :], places)[:, 0, :].astype(jnp.bfloat16)
    latent_normed = rms_scaled(latent, latent_gain).astype(jnp.bfloat16)
    key_first = jnp.dot(latent_normed, key_up_first, preferred_element_type=jnp.float32).astype(jnp.bfloat16)
    key_second = jnp.dot(latent_normed, key_up_second, preferred_element_type=jnp.float32).astype(jnp.bfloat16)
    value_first = jnp.dot(latent_normed, value_up_first, preferred_element_type=jnp.float32).astype(jnp.bfloat16)
    value_second = jnp.dot(latent_normed, value_up_second, preferred_element_type=jnp.float32).astype(jnp.bfloat16)
    attended_first = attend_group(queries_first, key_first, key_turned, value_first, (NA + ROPE) ** (-0.5))
    attended_second = attend_group(queries_second, key_second, key_turned, value_second, (NB + ROPE) ** (-0.5))
    set_first = attended_first.shape[1] // N_TP
    set_second = attended_second.shape[1] // N_TP
    projected = jnp.zeros((total, residual.shape[1]), jnp.float32)
    for index in range(N_TP):
        partial_value = jnp.dot(attended_first[:, index * set_first:(index + 1) * set_first], out_first[index * set_first:(index + 1) * set_first], preferred_element_type=jnp.float32)
        partial_value = partial_value + jnp.dot(attended_second[:, index * set_second:(index + 1) * set_second], out_second[index * set_second:(index + 1) * set_second], preferred_element_type=jnp.float32)
        projected = projected + lax.optimization_barrier(partial_value.astype(jnp.bfloat16)).astype(jnp.float32)
    middle = (residual.astype(jnp.float32) + projected).astype(jnp.bfloat16)
    normed = rms_scaled(middle, expert_gain).astype(jnp.bfloat16)
    route_weight = jax.nn.softmax(route_scores, axis=-1)
    experts = gate_weight.shape[0]
    topk = route_experts.shape[1]
    block_rows = total // (N_SP * N_TP)
    blocks = total // block_rows
    chosen = route_experts.reshape(blocks, block_rows * topk)
    hits = (chosen[..., None] == jnp.arange(experts, dtype=jnp.int32)).astype(jnp.int32)
    ranks = lax.optimization_barrier(jnp.sum((jnp.cumsum(hits, axis=1) - hits) * hits, axis=-1))
    slot_place = jnp.arange(blocks, dtype=jnp.int32)[:, None] * CAP + ranks
    owners = jnp.broadcast_to(places.reshape(blocks, block_rows, 1), (blocks, block_rows, topk)).reshape(blocks, -1)
    table = jnp.full((experts, blocks * CAP), total, jnp.int32)
    table = table.at[chosen.reshape(-1), slot_place.reshape(-1)].set(owners.reshape(-1))
    padded = jnp.concatenate([normed, jnp.zeros((1, normed.shape[1]), jnp.bfloat16)], axis=0)

    def run_expert(operands):
        slots, gate_part, up_part, down_part = operands
        rows = padded[slots]
        gate = jnp.dot(rows, gate_part, preferred_element_type=jnp.float32)
        upward = jnp.dot(rows, up_part, preferred_element_type=jnp.float32)
        activated = clamped_unit(gate, upward).astype(jnp.bfloat16)
        unit_set = activated.shape[1] // N_TP
        parts = jnp.einsum('snf,nfd->snd', activated.reshape(-1, N_TP, unit_set).astype(jnp.float32), down_part.reshape(N_TP, unit_set, -1).astype(jnp.float32))
        rounded = lax.optimization_barrier(parts.astype(jnp.bfloat16)).astype(jnp.float32)
        return lax.optimization_barrier(jnp.sum(rounded, axis=1)).astype(jnp.bfloat16)
    results = lax.map(run_expert, (table, gate_weight, up_weight, down_weight))
    picked = results[chosen.reshape(-1), slot_place.reshape(-1)].reshape(total, topk, -1).astype(jnp.float32)
    mixture = lax.optimization_barrier(jnp.sum(route_weight[..., None] * picked, axis=1))
    return (middle.astype(jnp.float32) + mixture).astype(jnp.bfloat16)
```

```python
import functools

import jax
import jax.numpy as jnp
from jax import lax
from jax.experimental import pallas as pl
from jax.experimental.pallas import tpu as pltpu
from jax.sharding import PartitionSpec as P

NA = 64
NB = 128
ROPE = 32
CAP = 3


norm_epsilon = 1e-06
rotary_base = 10000.0
clamp_limit = 7.0
sigmoid_slope = 1.702
masked_score = -1e30


def rotate(values, positions):
    half = values.shape[-1] // 2
    inverse = rotary_base ** (-jnp.arange(half, dtype=jnp.float32) / half)
    angles = positions.astype(jnp.float32)[:, None, None] * inverse[None, None, :]
    cosine = jnp.cos(angles)
    sine = jnp.sin(angles)
    first = values[..., :half]
    second = values[..., half:]
    return jnp.concatenate(
        [first * cosine - second * sine, second * cosine + first * sine], axis=-1
    )


def rms_scaled(values, gain):
    wide = values.astype(jnp.float32)
    return wide * lax.rsqrt(jnp.mean(wide * wide, axis=-1, keepdims=True) + norm_epsilon) * gain


def turned_queries(query, nope, positions):
    shaped = query.reshape(query.shape[0], query.shape[1] // (nope + ROPE), nope + ROPE)
    turned = rotate(shaped[..., nope:].astype(jnp.float32), positions).astype(jnp.bfloat16)
    return jnp.concatenate([shaped[..., :nope], turned], axis=-1)


def clamped_unit(gate, upward):
    limited = jnp.minimum(gate, clamp_limit)
    bounded = jnp.clip(upward, -clamp_limit, clamp_limit)
    return (bounded + 1.0) * limited * jax.nn.sigmoid(sigmoid_slope * limited)


def slot_numbers(chosen, experts):
    hits = (chosen[..., None] == jnp.arange(experts, dtype=jnp.int32)).astype(jnp.int32)
    before = jnp.cumsum(hits, axis=-2) - hits
    return chosen * CAP + jnp.sum(before * hits, axis=-1)


def fold_group(state, queries, key_nope, key_turned, values, query_places, scale):
    running, denominator, numerator = state
    heads = queries.shape[1]
    nope = queries.shape[2] - key_turned.shape[1]
    keys = key_nope.reshape(key_nope.shape[0], heads, nope)
    value_rows = values.reshape(values.shape[0], heads, values.shape[1] // heads)
    score = jnp.einsum(
        "qhd,khd->qhk", queries[..., :nope], keys, preferred_element_type=jnp.float32
    )
    score = score + jnp.einsum(
        "qhr,kr->qhk", queries[..., nope:], key_turned, preferred_element_type=jnp.float32
    )
    score = score * scale
    key_places = jnp.arange(keys.shape[0], dtype=jnp.int32)
    allowed = (query_places[:, None] >= key_places[None, :])[:, None, :]
    score = jnp.where(allowed, score, masked_score)
    highest = jnp.maximum(running, jnp.max(score, axis=-1))
    weights = jnp.where(allowed, jnp.exp(score - highest[..., None]), 0.0)
    denominator = jnp.sum(weights, axis=-1)
    numerator = jnp.einsum(
        "qhk,khd->qhd", weights.astype(jnp.bfloat16), value_rows, preferred_element_type=jnp.float32
    )
    return (highest, denominator, numerator)


def expert_hidden(rows, gate_weight, up_weight):
    gate = jnp.einsum("nsecd,edf->nsecf", rows, gate_weight, preferred_element_type=jnp.float32)
    upward = jnp.einsum("nsecd,edf->nsecf", rows, up_weight, preferred_element_type=jnp.float32)
    return clamped_unit(gate, upward).astype(jnp.bfloat16)


def slot_body(
    query_first,
    query_second,
    latent,
    key_rotary,
    latent_gain,
    key_up_first,
    value_up_first,
    key_up_second,
    value_up_second,
    out_first,
    out_second,
    residual,
    expert_gain,
    route_experts,
    route_scores,
    gate_weight,
    up_weight,
    down_weight,
):
    seq_rows = latent.shape[0]
    sets = lax.axis_size("tp")
    groups = lax.axis_size("sp")
    own_rows = seq_rows // sets
    topk = route_experts.shape[1]
    local_experts = gate_weight.shape[0]
    experts = local_experts * groups
    offset = lax.axis_index("sp") * seq_rows
    places = offset + jnp.arange(seq_rows, dtype=jnp.int32)
    last_place = offset + seq_rows - 1
    queries_first = turned_queries(query_first, NA, places)
    queries_second = turned_queries(query_second, NB, places)
    key_turned = rotate(key_rotary.astype(jnp.float32)[:, None, :], places)[:, 0, :].astype(
        jnp.bfloat16
    )
    latent_normed = rms_scaled(latent, latent_gain).astype(jnp.bfloat16)
    scale_first = (NA + ROPE) ** (-0.5)
    scale_second = (NB + ROPE) ** (-0.5)

    def attend(carry, parts):
        key_first, value_first, key_second, value_second, turned = parts
        return (
            fold_group(
                carry[0], queries_first, key_first, turned, value_first, places, scale_first
            ),
            fold_group(
                carry[1], queries_second, key_second, turned, value_second, places, scale_second
            ),
        )

    def initial(queries, value_width):
        shape = queries.shape[:2]
        return (
            jnp.full(shape, masked_score, jnp.float32),
            jnp.zeros(shape, jnp.float32),
            jnp.zeros(shape + (value_width,), jnp.float32),
        )

    start_state = (
        initial(queries_first, value_up_first.shape[1] // queries_first.shape[1]),
        initial(queries_second, value_up_second.shape[1] // queries_second.shape[1]),
    )
    key_first, value_first, key_second, value_second = tuple(
        (
            jnp.dot(latent_normed, weight, preferred_element_type=jnp.float32).astype(jnp.bfloat16)
            for weight in (key_up_first, value_up_first, key_up_second, value_up_second)
        )
    )
    parts = (
        lax.all_gather(key_first, "sp", axis=0, tiled=True),
        lax.all_gather(value_first, "sp", axis=0, tiled=True),
        lax.all_gather(key_second, "sp", axis=0, tiled=True),
        lax.all_gather(value_second, "sp", axis=0, tiled=True),
        lax.all_gather(key_turned, "sp", axis=0, tiled=True),
    )
    state = lax.cond(
        jnp.int32(0) <= last_place,
        lambda inner: attend(inner, parts),
        lambda inner: inner,
        start_state,
    )
    first_state, second_state = state
    attended_first = (
        (first_state[2] / first_state[1][..., None]).astype(jnp.bfloat16).reshape(seq_rows, -1)
    )
    attended_second = (
        (second_state[2] / second_state[1][..., None]).astype(jnp.bfloat16).reshape(seq_rows, -1)
    )
    own_start = lax.axis_index("tp") * own_rows
    slot_range = jnp.arange(experts * CAP, dtype=jnp.int32)
    projected = lax.psum_scatter(
        (
            jnp.dot(attended_first, out_first, preferred_element_type=jnp.float32)
            + jnp.dot(attended_second, out_second, preferred_element_type=jnp.float32)
        ).astype(jnp.bfloat16),
        "tp",
        scatter_dimension=0,
        tiled=True,
    ).astype(jnp.float32)
    own_residual = lax.dynamic_slice_in_dim(residual, own_start, own_rows, 0)
    middle = (own_residual.astype(jnp.float32) + projected).astype(jnp.bfloat16)
    normed = rms_scaled(middle, expert_gain).astype(jnp.bfloat16)
    own_ids = lax.dynamic_slice_in_dim(route_experts, own_start, own_rows, 0).reshape(-1)
    own_slots = slot_numbers(own_ids, experts)
    picks = (own_slots[:, None] == slot_range).reshape(own_rows, topk, experts * CAP)
    selected = jnp.sum(picks.astype(jnp.float32), axis=1).astype(jnp.bfloat16)
    outgoing = jnp.einsum("ts,td->sd", selected, normed, preferred_element_type=jnp.float32).astype(
        jnp.bfloat16
    )
    outgoing = outgoing.reshape(groups, local_experts, CAP, outgoing.shape[-1])
    arrived = lax.all_to_all(outgoing, "sp", split_axis=0, concat_axis=0, tiled=True)
    activated = expert_hidden(
        lax.all_gather(arrived[None], "tp", axis=0, tiled=True), gate_weight, up_weight
    )
    flat_hidden = activated.reshape(sets * groups, local_experts, CAP, activated.shape[-1])
    summed = lax.psum_scatter(
        jnp.einsum(
            "secf,efd->secd", flat_hidden, down_weight, preferred_element_type=jnp.float32
        ).astype(jnp.bfloat16),
        "tp",
        scatter_dimension=0,
        tiled=True,
    )
    returned = lax.all_to_all(summed, "sp", split_axis=0, concat_axis=0, tiled=True)
    expert_out = returned.reshape(experts * CAP, returned.shape[-1]).astype(jnp.float32)
    own_scores = lax.dynamic_slice_in_dim(route_scores, own_start, own_rows, 0)
    route_weight = jax.nn.softmax(own_scores, axis=-1)
    matches = own_slots.reshape(own_rows, topk)[..., None] == slot_range
    combine = jnp.sum(jnp.where(matches, route_weight[..., None], 0.0), axis=1)
    mixture = jnp.dot(combine, expert_out, precision=lax.Precision.HIGHEST)
    return (middle.astype(jnp.float32) + mixture).astype(jnp.bfloat16)


MESH = pl.DeviceIdType.MESH
VMEM = pl.BlockSpec(memory_space=pltpu.VMEM)
TILE_TOKENS = 256


def places_of(axes):
    return {axis: lax.axis_index(axis) for axis in axes}


def bit_of(place, step):
    axis, mask = step
    return (place[axis] // mask) % 2


def partner_of(place, step):
    axis, mask = step
    return {axis: place[axis] + mask * (1 - 2 * bit_of(place, step))}


def greet(place, steps):
    barrier = pltpu.get_barrier_semaphore()
    for step in steps:
        pl.semaphore_signal(
            barrier, inc=1, device_id=partner_of(place, step), device_id_type=MESH
        )
    pl.semaphore_wait(barrier, len(steps))


def cube_steps(sp, tp):
    core = [("tp", 1)] if tp > 1 else []
    first = [("tp", 2)] if tp > 2 else []
    rest = [("tp", 1 << i) for i in range(2, tp.bit_length() - 1)]
    across = [("sp", 1 << i) for i in range(sp.bit_length() - 1)]
    return core, first, rest, across


def weight_of(step, widths):
    axis, mask = step
    return mask * (widths if axis == "sp" else 1)


def base_of(place, fixed, width):
    total = jnp.int32(0)
    for step in fixed:
        total = total + bit_of(place, step) * weight_of(step, width)
    return total


def offsets_of(free, width):
    found = [0]
    for step in free:
        found = found + [one + weight_of(step, width) for one in found]
    return found


def block_rows_of(index, rows):
    return pl.ds(pl.multiple_of(index * rows, rows), rows)


def gather_kernel(orders, width, x_ref, out_ref, send_sem, recv_sem, own_sem):
    place = places_of(("sp", "tp"))
    steps = orders[0]
    rows = x_ref.shape[0]
    cols = x_ref.shape[1] // len(orders)
    greet(place, steps)
    own = pltpu.make_async_copy(
        x_ref, out_ref.at[block_rows_of(base_of(place, steps, width), rows), :], own_sem
    )
    own.start()

    def columns(part):
        return pl.ds(part * cols, cols)

    def start(part, number):
        order = orders[part]
        base = base_of(place, order[number:], width)
        for offset in offsets_of(order[:number], width):
            spot = out_ref.at[block_rows_of(base + offset, rows), columns(part)]
            source = x_ref.at[:, columns(part)] if number == 0 else spot
            pltpu.make_async_remote_copy(
                src_ref=source,
                dst_ref=spot,
                send_sem=send_sem.at[part, number],
                recv_sem=recv_sem.at[part, number],
                device_id=partner_of(place, order[number]),
                device_id_type=MESH,
            ).start()

    def drain(part, number, sem):
        whole = out_ref.at[pl.ds(0, rows << number), columns(part)]
        pltpu.make_async_copy(whole, whole, sem.at[part, number]).wait()

    for part in range(len(orders)):
        start(part, 0)
    own.wait()
    for wave in range(len(steps) + 1):
        for part in range(len(orders)):
            number = wave - part // 2 % 2
            if number < 0 or number >= len(steps):
                continue
            drain(part, number, recv_sem)
            if number + 1 < len(steps):
                start(part, number + 1)
    for part in range(len(orders)):
        for number in range(len(steps)):
            drain(part, number, send_sem)


def gather_blocks(x, orders, width, count, collective_id):
    rows, depth = x.shape
    parts, stages = len(orders), len(orders[0])
    return pl.pallas_call(
        functools.partial(gather_kernel, orders, width),
        out_shape=jax.ShapeDtypeStruct((rows * count, depth), x.dtype),
        in_specs=[VMEM],
        out_specs=VMEM,
        scratch_shapes=[
            pltpu.SemaphoreType.DMA((parts, stages)),
            pltpu.SemaphoreType.DMA((parts, stages)),
            pltpu.SemaphoreType.DMA,
        ],
        compiler_params=pltpu.CompilerParams(
            collective_id=collective_id, has_side_effects=True, vmem_limit_bytes=40 << 20
        ),
        name="gather_blocks",
    )(x)


def scatter_kernel(
    orders, width, rows, x_ref, out_ref, total_ref, landing_ref, send_sem, recv_sem
):
    place = places_of(("sp", "tp"))
    stages = len(orders[0])
    cols = x_ref.shape[1] // len(orders)
    greet(place, orders[0])
    spots = [0]
    for number in range(stages):
        spots.append(spots[-1] + (1 << (stages - 1 - number)))

    def columns(part):
        return pl.ds(part * cols, cols)

    def start(part, number):
        order = orders[part]
        step = order[number]
        source = x_ref if number == 0 else total_ref
        base = base_of(place, order[:number], width)
        base = base + (1 - bit_of(place, step)) * weight_of(step, width)
        for slot, offset in enumerate(offsets_of(order[number + 1 :], width)):
            pltpu.make_async_remote_copy(
                src_ref=source.at[block_rows_of(base + offset, rows), columns(part)],
                dst_ref=landing_ref.at[pl.ds((spots[number] + slot) * rows, rows), columns(part)],
                send_sem=send_sem.at[part, number],
                recv_sem=recv_sem.at[part, number],
                device_id=partner_of(place, step),
                device_id_type=MESH,
            ).start()

    def drain(part, number, sem):
        count = 1 << (stages - 1 - number)
        whole = landing_ref.at[pl.ds(spots[number] * rows, count * rows), columns(part)]
        pltpu.make_async_copy(whole, whole, sem.at[part, number]).wait()

    def add(part, number):
        order = orders[part]
        source = x_ref if number == 0 else total_ref
        base = base_of(place, order[: number + 1], width)
        for slot, offset in enumerate(offsets_of(order[number + 1 :], width)):
            here = block_rows_of(base + offset, rows)
            there = pl.ds((spots[number] + slot) * rows, rows)
            value = source[here, columns(part)].astype(jnp.float32) + landing_ref[
                there, columns(part)
            ].astype(jnp.float32)
            if number + 1 < stages:
                total_ref[here, columns(part)] = value.astype(total_ref.dtype)
            else:
                out_ref[:, columns(part)] = value

    for part in range(len(orders)):
        start(part, 0)
    for wave in range(stages + 1):
        for part in range(len(orders)):
            number = wave - part // 2 % 2
            if number < 0 or number >= stages:
                continue
            drain(part, number, recv_sem)
            add(part, number)
            if number + 1 < stages:
                start(part, number + 1)
    for part in range(len(orders)):
        for number in range(stages):
            drain(part, number, send_sem)


def scatter_blocks(x, orders, width, count, collective_id):
    rows = x.shape[0] // count
    depth = x.shape[1]
    parts, stages = len(orders), len(orders[0])
    return pl.pallas_call(
        functools.partial(scatter_kernel, orders, width, rows),
        out_shape=jax.ShapeDtypeStruct((rows, depth), jnp.float32),
        in_specs=[VMEM],
        out_specs=VMEM,
        scratch_shapes=[
            pltpu.VMEM(x.shape, x.dtype),
            pltpu.VMEM(((count - 1) * rows, depth), x.dtype),
            pltpu.SemaphoreType.DMA((parts, stages)),
            pltpu.SemaphoreType.DMA((parts, stages)),
        ],
        compiler_params=pltpu.CompilerParams(
            collective_id=collective_id, has_side_effects=True, vmem_limit_bytes=40 << 20
        ),
        name="scatter_blocks",
    )(x)


def exchange_kernel(latent_ref, turn_ref, route_ref, l_out, t_out, r_out, send_sem, recv_sem, own_sem):
    place = places_of(("sp", "tp"))
    across, core = ("sp", 1), ("tp", 1)
    greet(place, (across, core))
    half = latent_ref.shape[0] // 2
    side = bit_of(place, core)
    me = place["sp"]
    other = 1 - me
    pairs = ((latent_ref, l_out), (turn_ref, t_out))
    mine = pl.ds(pl.multiple_of(side * half, half), half)
    crossing = []
    for number, (source, target) in enumerate(pairs):
        crossing.append(
            pltpu.make_async_remote_copy(
                src_ref=source.at[mine, :],
                dst_ref=target.at[me, mine, :],
                send_sem=send_sem.at[number],
                recv_sem=recv_sem.at[number],
                device_id=partner_of(place, across),
                device_id_type=MESH,
            )
        )
    crossing.append(
        pltpu.make_async_remote_copy(
            src_ref=route_ref,
            dst_ref=r_out.at[me],
            send_sem=send_sem.at[2],
            recv_sem=recv_sem.at[2],
            device_id=partner_of(place, across),
            device_id_type=MESH,
        )
    )
    for copy in crossing:
        copy.start()
    kept = [
        pltpu.make_async_copy(source, target.at[me], own_sem.at[number])
        for number, (source, target) in enumerate(pairs + ((route_ref, r_out),))
    ]
    for copy in kept:
        copy.start()
    passing = []
    for number, (source, target) in enumerate(pairs):
        crossing[number].wait_recv()
        spot = target.at[other, mine, :]
        copy = pltpu.make_async_remote_copy(
            src_ref=spot,
            dst_ref=spot,
            send_sem=send_sem.at[3 + number],
            recv_sem=recv_sem.at[3 + number],
            device_id=partner_of(place, core),
            device_id_type=MESH,
        )
        copy.start()
        passing.append(copy)
    crossing[2].wait_recv()
    for copy in crossing:
        copy.wait_send()
    for copy in kept + passing:
        copy.wait()


def exchange(latent, turn, route, collective_id):
    return pl.pallas_call(
        exchange_kernel,
        out_shape=tuple(
            jax.ShapeDtypeStruct((2,) + one.shape, one.dtype) for one in (latent, turn, route)
        ),
        in_specs=[VMEM] * 3,
        out_specs=(VMEM,) * 3,
        scratch_shapes=[
            pltpu.SemaphoreType.DMA((5,)),
            pltpu.SemaphoreType.DMA((5,)),
            pltpu.SemaphoreType.DMA((3,)),
        ],
        compiler_params=pltpu.CompilerParams(collective_id=collective_id, has_side_effects=True),
        name="exchange",
    )(latent, turn, route)


def expert_kernel(pitch, x_ref, code_ref, gate_ref, up_ref, down_ref, out_ref, rows_ref, scale_ref):
    index = pl.program_id(0)
    experts = pl.num_programs(0)
    tiles, count, _, depth = rows_ref.shape
    span = count * pitch
    tokens = x_ref.shape[0] // tiles

    def hits(tile, choice):
        wanted = code_ref[tile, pl.ds(choice, 1), :]
        slots = lax.broadcasted_iota(jnp.int32, (span, tokens), 0)
        return slots == wanted.astype(jnp.int32)

    @pl.when(index == 0)
    def _():
        for tile in range(tiles):
            first, second = hits(tile, 0), hits(tile, 1)
            chosen = jnp.where(first | second, 1.0, 0.0).astype(jnp.bfloat16)
            picked = jnp.dot(
                chosen,
                x_ref[pl.ds(tile * tokens, tokens), :],
                preferred_element_type=jnp.float32,
            ).astype(jnp.bfloat16)
            rows_ref[tile] = picked.reshape(count, pitch, depth)
            share = jnp.where(first, code_ref[tile, pl.ds(2, 1), :], 0.0) + jnp.where(
                second, code_ref[tile, pl.ds(3, 1), :], 0.0
            )
            scale_ref[tile] = jnp.sum(share, axis=1, keepdims=True).reshape(count, pitch, 1)

    rows = rows_ref[:, index].reshape(tiles * pitch, depth)
    gate = jnp.dot(rows, gate_ref[0], preferred_element_type=jnp.float32)
    upward = jnp.dot(rows, up_ref[0], preferred_element_type=jnp.float32)
    activated = clamped_unit(gate, upward).astype(jnp.bfloat16)
    result = jnp.dot(activated, down_ref[0], preferred_element_type=jnp.float32)
    scaled = result * scale_ref[:, index].reshape(tiles * pitch, 1)
    rows_ref[:, index] = scaled.astype(jnp.bfloat16).reshape(tiles, pitch, depth)

    @pl.when(index == experts - 1)
    def _():
        for tile in range(tiles):
            chosen = jnp.where(hits(tile, 0) | hits(tile, 1), 1.0, 0.0).astype(jnp.bfloat16)
            out_ref[pl.ds(tile * tokens, tokens), :] = lax.dot_general(
                chosen,
                rows_ref[tile].reshape(span, depth),
                (((0,), (0,)), ((), ())),
                preferred_element_type=jnp.float32,
            ).astype(jnp.bfloat16)


def run_experts(tokens, codes, gate_weight, up_weight, down_weight, pitch):
    experts, depth, units = gate_weight.shape
    tiles = codes.shape[0]
    return pl.pallas_call(
        functools.partial(expert_kernel, pitch),
        grid=(experts,),
        out_shape=jax.ShapeDtypeStruct(tokens.shape, jnp.bfloat16),
        in_specs=[
            pl.BlockSpec(tokens.shape, lambda i: (0, 0)),
            pl.BlockSpec(codes.shape, lambda i: (0, 0, 0)),
            pl.BlockSpec((1, depth, units), lambda i: (i, 0, 0)),
            pl.BlockSpec((1, depth, units), lambda i: (i, 0, 0)),
            pl.BlockSpec((1, units, depth), lambda i: (i, 0, 0)),
        ],
        out_specs=pl.BlockSpec(tokens.shape, lambda i: (0, 0)),
        scratch_shapes=[
            pltpu.VMEM((tiles, experts, pitch, depth), jnp.bfloat16),
            pltpu.VMEM((tiles, experts, pitch, 1), jnp.float32),
        ],
        compiler_params=pltpu.CompilerParams(
            dimension_semantics=("arbitrary",), vmem_limit_bytes=56 << 20
        ),
        name="run_experts",
    )(tokens, codes, gate_weight, up_weight, down_weight)


def attended_heads(queries, nope, keys, turned, values, allowed, scale):
    heads = queries.shape[1]
    wide = keys.reshape(keys.shape[0], heads, nope)
    shared = jnp.broadcast_to(turned[:, None, :], (turned.shape[0], heads, turned.shape[1]))
    whole = jnp.concatenate([wide, shared], axis=-1)
    value_rows = values.reshape(values.shape[0], heads, values.shape[1] // heads)
    score = jnp.einsum("qhd,khd->hqk", queries, whole, preferred_element_type=jnp.float32) * scale
    score = jnp.where(allowed, score, masked_score)
    highest = jnp.max(score, axis=-1, keepdims=True)
    weights = jnp.exp(score - highest)
    denominator = jnp.sum(weights, axis=-1)
    numerator = jnp.einsum(
        "hqk,khd->hqd", weights.astype(jnp.bfloat16), value_rows, preferred_element_type=jnp.float32
    )
    attended = (numerator / denominator[..., None]).astype(jnp.bfloat16)
    return jnp.swapaxes(attended, 0, 1).reshape(attended.shape[1], -1)


def token_body(
    query_first,
    query_second,
    latent,
    key_rotary,
    latent_gain,
    key_up_first,
    value_up_first,
    key_up_second,
    value_up_second,
    out_first,
    out_second,
    residual,
    expert_gain,
    route_experts,
    route_scores,
    gate_weight,
    up_weight,
    down_weight,
):
    seq_rows = latent.shape[0]
    sets = lax.axis_size("tp")
    groups = lax.axis_size("sp")
    own_rows = seq_rows // sets
    local_experts = gate_weight.shape[0]
    total = groups * seq_rows
    me = lax.axis_index("sp")
    core, first, rest, across = cube_steps(groups, sets)
    span_blocks = TILE_TOKENS // own_rows
    pitch = -(-span_blocks * CAP // 16) * 16

    chosen = route_experts.reshape(sets, -1)
    earlier = jnp.tril(jnp.ones((chosen.shape[1],) * 2, jnp.float32), -1)
    same = (chosen[:, :, None] == chosen[:, None, :]).astype(jnp.float32)
    rank = jnp.sum(same * earlier, axis=-1)
    spot = ((jnp.arange(sets, dtype=jnp.int32) % span_blocks) * CAP).astype(jnp.float32)
    code = chosen.astype(jnp.float32) * pitch + spot[:, None] + rank
    code = code.reshape(seq_rows, -1).T
    share = jax.nn.softmax(route_scores, axis=-1).T
    route = jnp.concatenate([code, share, code, share], axis=0)

    latents, turns, routes = exchange(latent, key_rotary, route, 0)

    places = me * seq_rows + jnp.arange(seq_rows, dtype=jnp.int32)
    all_places = jnp.arange(total, dtype=jnp.int32)
    queries_first = turned_queries(query_first, NA, places)
    queries_second = turned_queries(query_second, NB, places)
    turned = rotate(
        turns.reshape(total, -1).astype(jnp.float32)[:, None, :], all_places
    )[:, 0, :].astype(jnp.bfloat16)
    latent_normed = rms_scaled(latents.reshape(total, -1), latent_gain).astype(jnp.bfloat16)
    key_first, value_first, key_second, value_second = tuple(
        jnp.dot(latent_normed, weight, preferred_element_type=jnp.float32).astype(jnp.bfloat16)
        for weight in (key_up_first, value_up_first, key_up_second, value_up_second)
    )
    allowed = (places[:, None] >= all_places[None, :])[None]
    attended_first = attended_heads(
        queries_first, NA, key_first, turned, value_first, allowed, (NA + ROPE) ** (-0.5)
    )
    attended_second = attended_heads(
        queries_second, NB, key_second, turned, value_second, allowed, (NB + ROPE) ** (-0.5)
    )
    partial = (
        jnp.dot(attended_first, out_first, preferred_element_type=jnp.float32)
        + jnp.dot(attended_second, out_second, preferred_element_type=jnp.float32)
    ).astype(jnp.bfloat16)
    one, two = tuple(core + first + rest), tuple(core + rest + first)
    projected = scatter_blocks(partial, (one, two, one, one), sets, sets, 1)
    own_start = lax.axis_index("tp") * own_rows
    own_residual = lax.dynamic_slice_in_dim(residual, own_start, own_rows, 0)
    middle = (own_residual.astype(jnp.float32) + projected).astype(jnp.bfloat16)
    normed = rms_scaled(middle, expert_gain).astype(jnp.bfloat16)
    ladder = rest[::-1]
    one = tuple(ladder + across + first + core)
    two = tuple(ladder + first + across + core)
    tokens = gather_blocks(normed, (one, two, one, two), sets, groups * sets, 2)

    tiles = total // TILE_TOKENS
    codes = jnp.swapaxes(routes, 0, 1).reshape(8, total)
    shift = jnp.array([1.0, 1.0, 0.0, 0.0, 1.0, 1.0, 0.0, 0.0], jnp.float32)
    codes = codes - (shift * (me * local_experts * pitch).astype(jnp.float32))[:, None]
    codes = jnp.swapaxes(codes.reshape(8, tiles, TILE_TOKENS), 0, 1)
    mixed = run_experts(tokens, codes, gate_weight, up_weight, down_weight, pitch)
    one, two = one[::-1], two[::-1]
    mixture = scatter_blocks(mixed, (one, two, one, two), sets, groups * sets, 3)
    return (middle.astype(jnp.float32) + mixture).astype(jnp.bfloat16)


def solution(mesh):
    in_specs = (
        P("sp", "tp"),
        P("sp", "tp"),
        P("sp", None),
        P("sp", None),
        P(),
        P(None, "tp"),
        P(None, "tp"),
        P(None, "tp"),
        P(None, "tp"),
        P("tp", None),
        P("tp", None),
        P("sp", None),
        P(),
        P("sp", None),
        P("sp", None),
        P("sp", None, "tp"),
        P("sp", None, "tp"),
        P("sp", "tp", None),
    )
    out_specs = P(("sp", "tp"), None)
    groups, sets = mesh.shape["sp"], mesh.shape["tp"]
    small = groups == 2 and sets & (sets - 1) == 0 and sets > 2

    def body(*arguments):
        fits = small and arguments[2].shape[0] * groups <= 1024
        return (token_body if fits else slot_body)(*arguments)

    return jax.shard_map(body, mesh=mesh, in_specs=in_specs, out_specs=out_specs, check_vma=False)
```
